32 devices in a mesh: sp: 16 (over z, y, x), tp: 2 (over core).
Axes of the slice: x: 2, y: 2, z: 4, core: 2. Of those that a mesh axis runs over, the one named last changes fastest.
Arguments:
- out_grad: bfloat16 [3584, 2048], P('sp'), may hold values from -8 to 8
- routes: int32 [3584, 2], P('sp'), may hold values from 0 to 15, all different within a row; in each aligned block of 224 rows (0 to 223, 224 to 447, ...) at most 70 rows name the same one
- route_weights: float32 [3584, 2], P('sp'), may hold values from 0.5 to 2
- routed_rows: bfloat16 [16, 16, 70, 2048], P('sp'), may hold values from -6 to 6
- gate_weight: bfloat16 [16, 2048, 1024], P('sp', None, 'tp'), may hold values from -0.125 to 0.125
- up_weight: bfloat16 [16, 2048, 1024], P('sp', None, 'tp'), may hold values from -0.125 to 0.125
- down_weight: bfloat16 [16, 1024, 2048], P('sp', 'tp'), may hold values from -0.1875 to 0.1875
- values: bfloat16 [3584, 1024], P('sp', 'tp'), may hold values from -0.625 to 0.625
- key_side: bfloat16 [3584, 512], P('sp', 'tp'), may hold values from -0.625 to 0.625
- query_side: bfloat16 [3584, 512], P('sp', 'tp'), may hold values from -0.625 to 0.625
- decay_log: float32 [16, 3584], P('tp', 'sp'), may hold values from -0.09 to 0, as said below
- gate_in: bfloat16 [3584, 1024], P('sp', 'tp'), may hold values from -6 to 6
- entry_states: float32 [16, 16, 64, 128], P('sp', 'tp'), may hold values from -6 to 6
- out_weight: bfloat16 [2048, 1024], P(None, 'tp'), may hold values from -0.1875 to 0.1875
Outputs:
- grad_hidden: bfloat16 [3584, 2048], P('sp')
- grad_gate_weight: bfloat16 [16, 2048, 1024], P('sp', None, 'tp')
- grad_up_weight: bfloat16 [16, 2048, 1024], P('sp', None, 'tp')
- grad_down_weight: bfloat16 [16, 1024, 2048], P('sp', 'tp')
- grad_out_weight: float32 [2048, 1024], P('sp', 'tp')
- grad_values: bfloat16 [3584, 1024], P('sp', 'tp')
- grad_key_side: bfloat16 [3584, 512], P('sp', 'tp')
- grad_query_side: bfloat16 [3584, 512], P('sp', 'tp')
- grad_decay: float32 [16, 3584], P('tp', 'sp')
- grad_gate_in: bfloat16 [3584, 1024], P('sp', 'tp')
The draws below stay inside these ranges and needn't reach their ends.
Inputs may be any that keep to these rules, and one draw needn't show every extreme that they name: Each row names 2 different experts. Among the routes of one segment of 224 tokens no expert is named more than 70 times, and in some segments one expert is named exactly 70 times. `decay_log`: every entry is negative.
All inputs are finite; a program needn't handle non-finite values.
Results may differ from the reference program's by a relative error of at most 0.0072.
Values may be sent and summed in bfloat16 or wider, within the bound.
A program may use at most 128 MiB of HBM per device.

```python
import math
import jax
import jax.numpy as jnp
import numpy as np
from jax import lax

D = 2048
HEADS = 16
HEAD_DIM = 64
GROUPS = 4
NSTATE = 128
INNER = 1024
FE = 1024
TOP = 2
EXPERTS = 16
TOK_DEV = 224
TOKENS = 3584
CAP = 70
N_SP = 16
N_TP = 2


def draw_decay_log(key, part):
    keys = jax.random.split(key, 5)
    fast_share = 0.5
    fast = jax.random.uniform(keys[0], (HEADS,), jnp.float32) < fast_share
    slow_rate = math.log(10.0) / TOKENS * jnp.exp(jax.random.uniform(keys[1], (HEADS,), jnp.float32, math.log(0.15), math.log(0.6)))
    fast_rate = 1.0 / jax.random.uniform(keys[2], (HEADS,), jnp.float32, 30.0, 100.0)
    rate = jnp.where(fast, fast_rate, slow_rate)
    device_factor = jnp.repeat(jnp.exp(jax.random.uniform(keys[3], (TOKENS // TOK_DEV,), jnp.float32, math.log(0.5), math.log(2.0))), TOK_DEV)
    token_factor = jax.random.uniform(keys[4], (HEADS, TOKENS), jnp.float32, 0.7, 1.3)
    return -(rate[:, None] * device_factor[None, :] * token_factor)


def spiked(drawn, key, source, target, shards_of, factor):
    def block_of(dim):
        return (jnp.arange(drawn.shape[dim]) // (drawn.shape[dim] // shards_of)).reshape((-1,) + (1,) * (drawn.ndim - 1 - dim))

    one_side = jax.random.permutation(key, shards_of)[block_of(target)]
    second = (block_of(target) + shards_of // 2) % shards_of
    return jnp.where((block_of(source) == one_side) | (block_of(source) == second), factor * drawn, drawn)


def steps_of(rng, shape, cuts, low, largest):
    loudness = 1.0
    for position, shards_of in cuts:
        steps = jax.random.uniform(jax.random.fold_in(jax.random.fold_in(rng, 6), position), (shards_of,), jnp.float32, low / len(cuts), largest / len(cuts))
        loudness = loudness * jnp.repeat(jnp.exp(steps), shape[position] // shards_of).reshape((-1,) + (1,) * (len(shape) - 1 - position))
    return loudness


def shared_out(stream_key, own, number, rows, amount, top, most, lean):
    sequence = jax.random.permutation(stream_key, amount)
    packed, ordinary = portions_of(amount, rows * top, most, lean, True), portions_of(amount, rows * top, most, lean, False)
    places = jnp.arange(amount)

    def named(lengths, rotation):
        used = int((lengths > 0).sum())
        fixed = max(1, used // 4)
        shifted = fixed + (places - fixed + rotation * (used - fixed)) % max(1, amount - fixed)
        return jnp.zeros((amount,), jnp.int32).at[sequence[jnp.where(places < fixed, places, shifted)]].set(jnp.asarray(lengths, jnp.int32))

    lengths = jnp.where(number % 4 == 0, named(packed, number // 4), named(ordinary, number - number // 4 - 1))
    mixed = jax.random.permutation(jax.random.fold_in(own, 3), amount)
    source_of, sink = mixed[0:amount // 2 * 2:2], mixed[1:amount // 2 * 2:2]
    margin = jnp.minimum(lengths[source_of] - 1, most - lengths[sink]) // 2
    margin = jnp.where((source_of == sequence[0]) | (sink == sequence[0]) | (lengths[sink] == 0), 0, jnp.maximum(margin, 0))
    shifted = jax.random.randint(jax.random.fold_in(own, 4), (amount // 2,), 0, 1 << 20) % (margin + 1)
    lengths = lengths.at[source_of].add(-shifted).at[sink].add(shifted)
    members = jnp.searchsorted(jnp.cumsum(lengths), jnp.arange(rows * top), side="right").astype(jnp.int32)
    table = members.reshape(top, rows).T
    table = table[jax.random.permutation(jax.random.fold_in(own, 1), rows)]
    rotation = jax.random.randint(jax.random.fold_in(own, 2), (rows, 1), 0, top)
    return jnp.take_along_axis(table, (jnp.arange(top)[None, :] + rotation) % top, axis=1)


def portions_of(number_of, total, limit, lean, full):
    loads = [(1 << 20) // math.isqrt(standing ** lean) + 1 for standing in range(1, number_of + 1)]
    largest = limit if full else min(limit, max(-(-total // number_of), total * loads[0] // sum(loads)))
    least = 1 if total - largest >= number_of - 1 else 0
    holding, rest = [largest] + [least] * (number_of - 1), total - largest - least * (number_of - 1)
    while rest > 0:
        movable = [i for i in range(1, number_of) if holding[i] < largest] or [i for i in range(1, number_of) if holding[i] < limit]
        pool, budget = sum([loads[i] for i in movable]), rest
        for i in movable:
            more = min(limit - holding[i], max(1, budget * loads[i] // pool), rest)
            holding[i] = holding[i] + more
            rest = rest - more
    return np.array(holding)


def normal_values(stream_key, shape, scale, most, cuts=(), kind=jnp.bfloat16):
    factor_of = steps_of(stream_key, shape, cuts, -0.22, 0.18) if cuts else 1.0
    values = jax.random.normal(stream_key, shape, jnp.float32) * scale * factor_of
    return jnp.minimum(jnp.maximum(values, -most), most).astype(kind)


def heavy_noise(stream_key, extent, width, most, shards, heavy, kind=jnp.bfloat16):
    values = width * jax.random.normal(stream_key, extent, jnp.float32)
    if shards:
        values = values * steps_of(stream_key, extent, shards, -0.22, 0.18)
    return jnp.clip(spiked(values, jax.random.fold_in(stream_key, 3), *heavy), -most, most).astype(kind)


def setup_inputs(seed: int = 0) -> dict:
    key_list = jax.random.split(jax.random.key(seed), 15)
    out_grad = heavy_noise(key_list[0], (TOKENS, D), 1.0, 8.0, ((0, 16),), (0, 1, 16, 2.0))
    routes_keys = jax.random.split(jax.random.fold_in(key_list[1], 1), TOKENS // TOK_DEV)
    routes_turns = jax.random.permutation(jax.random.fold_in(key_list[1], 3), TOKENS // TOK_DEV)
    routes = jax.vmap(lambda own, number: shared_out(jax.random.fold_in(key_list[1], 2), own, number, TOK_DEV, EXPERTS, TOP, CAP, 1))(routes_keys, routes_turns).reshape((TOKENS, TOP))
    route_weights = jnp.clip(0.5 + 1.5 * jax.random.uniform(key_list[2], (TOKENS, TOP), jnp.float32) ** steps_of(key_list[2], (TOKENS, TOP), ((0, 16),), -0.2, 0.2), 0.5, 2.0)
    routed_rows = normal_values(key_list[3], (EXPERTS, N_SP, CAP, D), 1.0, 6.0, ((0, 16),))
    gate_weight = normal_values(key_list[4], (EXPERTS, D, FE), D ** -0.5, 0.125, ((0, 16), (2, 2)))
    up_weight = normal_values(key_list[5], (EXPERTS, D, FE), D ** -0.5, 0.125, ((0, 16), (2, 2)))
    down_weight = normal_values(key_list[6], (EXPERTS, FE, D), FE ** -0.5, 0.1875, ((0, 16), (1, 2)))
    values = normal_values(key_list[7], (TOKENS, INNER), 0.1, 0.625, ((0, 16), (1, 2)))
    key_side = normal_values(key_list[8], (TOKENS, GROUPS * NSTATE), 0.1, 0.625, ((0, 16), (1, 2)))
    query_side = normal_values(key_list[9], (TOKENS, GROUPS * NSTATE), 0.1, 0.625, ((0, 16), (1, 2)))
    decay_log = draw_decay_log(jax.random.fold_in(key_list[14], 71), 0)
    gate_in = normal_values(key_list[11], (TOKENS, INNER), 1.0, 6.0, ((0, 16), (1, 2)))
    entry_states = normal_values(key_list[12], (N_SP, HEADS, HEAD_DIM, NSTATE), 1.0, 6.0, ((0, 16), (1, 2)), jnp.float32)
    out_weight = normal_values(key_list[13], (D, INNER), INNER ** -0.5, 0.1875, ((1, 2),))
    return {"out_grad": out_grad, "routes": routes, "route_weights": route_weights, "routed_rows": routed_rows, "gate_weight": gate_weight, "up_weight": up_weight, "down_weight": down_weight, "values": values, "key_side": key_side, "query_side": query_side, "decay_log": decay_log, "gate_in": gate_in, "entry_states": entry_states, "out_weight": out_weight}


precise = lax.Precision.HIGHEST

def route_slots(routes_dev, expert_count):
    flat_routes = routes_dev.reshape(-1)
    onehot = (flat_routes[:, None] == jnp.arange(expert_count, dtype=jnp.int32)[None, :]).astype(jnp.int32)
    earlier = jnp.cumsum(onehot, axis=0) - onehot
    return lax.optimization_barrier(jnp.sum(earlier * onehot, axis=1)).astype(jnp.int32)

def block_forward(values, key_side, query_side, decay_log, gate_in, entry_state):
    length = values.shape[0]
    head_count = decay_log.shape[0]
    per_group = HEADS // GROUPS
    group_count = head_count // per_group
    grouped = values.reshape(length, group_count, per_group, HEAD_DIM)
    key_rows = key_side.reshape(length, group_count, NSTATE)
    query_rows = query_side.reshape(length, group_count, NSTATE)
    cumulative = jnp.cumsum(decay_log, axis=1)
    causal = jnp.tril(jnp.ones((length, length), bool))
    spread = cumulative[:, :, None] - cumulative[:, None, :]
    weights = jnp.where(causal, jnp.exp(jnp.where(causal, spread, 0.0)), 0.0)
    weights = weights.reshape(group_count, per_group, length, length)
    scores = jnp.einsum('tgn,sgn->gts', query_rows, key_rows, precision=precise)
    within = jnp.einsum('ghts,sghp->tghp', scores[:, None] * weights, grouped, precision=precise)
    carried = jnp.einsum('tgn,ghpn->tghp', query_rows, entry_state.reshape(group_count, per_group, HEAD_DIM, NSTATE), precision=precise)
    growth = jnp.exp(cumulative).reshape(group_count, per_group, length).transpose(2, 0, 1)
    core_out = (within + carried * growth[..., None]).reshape(length, head_count * HEAD_DIM)
    return core_out * jax.nn.silu(gate_in)

def end_state(values, key_side, decay_log, entry_state):
    length = values.shape[0]
    head_count = decay_log.shape[0]
    per_group = HEADS // GROUPS
    group_count = head_count // per_group
    grouped = values.reshape(length, group_count, per_group, HEAD_DIM)
    key_rows = key_side.reshape(length, group_count, NSTATE)
    cumulative = jnp.cumsum(decay_log, axis=1)
    final_sum = cumulative[:, -1]
    tail_decay = jnp.exp(final_sum[:, None] - cumulative).reshape(group_count, per_group, length)
    fresh_state = jnp.einsum('sgn,ghs,sghp->ghpn', key_rows, tail_decay, grouped, precision=precise)
    return jnp.exp(final_sum)[:, None, None] * entry_state + fresh_state.reshape(head_count, HEAD_DIM, NSTATE)

def reference(out_grad, routes, route_weights, routed_rows, gate_weight, up_weight, down_weight, values, key_side, query_side, decay_log, gate_in, entry_states, out_weight):
    route_count = TOKENS * TOP
    slot_index = jax.vmap(lambda device_routes: route_slots(device_routes, EXPERTS))(routes.reshape(N_SP, TOK_DEV, TOP)).reshape(-1)
    flat_routes = routes.reshape(-1)
    route_ids = jnp.arange(route_count, dtype=jnp.int32)
    source = (route_ids // (TOK_DEV * TOP)).astype(jnp.int32)
    owner_table = jnp.zeros((EXPERTS, N_SP, CAP), jnp.int32).at[flat_routes, source, slot_index].set(route_ids + 1)
    cot_rows = (route_weights[:, :, None] * out_grad.astype(jnp.float32)[:, None, :]).astype(jnp.bfloat16)
    cot_rows = cot_rows.reshape(route_count, D)
    span_width = FE // N_TP

    def expert_step(carried_sum, inputs):
        owner_e, rows_e, gate_e, up_e, down_e = inputs
        filled = (owner_e > 0).reshape(-1)
        picked = jnp.maximum(owner_e.reshape(-1) - 1, 0).astype(jnp.int32)
        cot_block = jnp.where(filled[:, None], cot_rows[picked], jnp.zeros((), jnp.bfloat16))
        row_block = rows_e.reshape(-1, D)
        gate_pre = jnp.dot(row_block, gate_e, preferred_element_type=jnp.float32)
        up_pre = jnp.dot(row_block, up_e, preferred_element_type=jnp.float32)
        act = (jax.nn.silu(gate_pre) * up_pre).astype(jnp.bfloat16)
        act_grad = jnp.dot(cot_block, down_e.T, preferred_element_type=jnp.float32)
        gate_sigmoid = jax.nn.sigmoid(gate_pre)
        gate_grad = (act_grad * up_pre * gate_sigmoid * (1.0 + gate_pre * (1.0 - gate_sigmoid))).astype(jnp.bfloat16)
        up_grad = (act_grad * jax.nn.silu(gate_pre)).astype(jnp.bfloat16)
        grad_down = jnp.dot(act.T, cot_block, preferred_element_type=jnp.float32).astype(jnp.bfloat16)
        grad_gate = jnp.dot(row_block.T, gate_grad, preferred_element_type=jnp.float32).astype(jnp.bfloat16)
        grad_up = jnp.dot(row_block.T, up_grad, preferred_element_type=jnp.float32).astype(jnp.bfloat16)
        back_rows = jnp.zeros((row_block.shape[0], D), jnp.float32)
        for span_index in range(N_TP):
            offset = span_index * span_width
            span_back = jnp.dot(gate_grad[:, offset:offset + span_width], gate_e[:, offset:offset + span_width].T, preferred_element_type=jnp.float32)
            span_back = span_back + jnp.dot(up_grad[:, offset:offset + span_width], up_e[:, offset:offset + span_width].T, preferred_element_type=jnp.float32)
            back_rows = back_rows + lax.optimization_barrier(span_back.astype(jnp.bfloat16)).astype(jnp.float32)
        back_rows = lax.optimization_barrier(back_rows.astype(jnp.bfloat16)).astype(jnp.float32)
        back_rows = jnp.where(filled[:, None], back_rows, 0.0)
        carried_sum = carried_sum.at[picked // TOP].add(back_rows)
        return (carried_sum, (grad_gate, grad_up, grad_down))
    moe_sum, (grad_gate_weight, grad_up_weight, grad_down_weight) = lax.scan(expert_step, jnp.zeros((TOKENS, D), jnp.float32), (owner_table, routed_rows, gate_weight, up_weight, down_weight))
    grad_hidden = (out_grad.astype(jnp.float32) + moe_sum).astype(jnp.bfloat16)
    mix_cot = jnp.dot(grad_hidden, out_weight, preferred_element_type=jnp.float32)

    def joint(value_seg, key_seg, query_seg, decay_seg, gate_seg, entry_state):
        return (block_forward(value_seg, key_seg, query_seg, decay_seg, gate_seg, entry_state), end_state(value_seg, key_seg, decay_seg, entry_state))

    def segment_step(state_cot, inputs):
        value_seg, key_seg, query_seg, decay_seg, gate_seg, entry_state, cot_seg = inputs
        (mixed_out, _), pull_back = jax.vjp(joint, value_seg, key_seg, query_seg, decay_seg, gate_seg, entry_state)
        grads = pull_back((cot_seg, state_cot))
        return (grads[5], (mixed_out, grads[0], grads[1], grads[2], grads[3], grads[4]))
    segment_inputs = (values.astype(jnp.float32).reshape(N_SP, TOK_DEV, INNER), key_side.astype(jnp.float32).reshape(N_SP, TOK_DEV, GROUPS * NSTATE), query_side.astype(jnp.float32).reshape(N_SP, TOK_DEV, GROUPS * NSTATE), decay_log.reshape(HEADS, N_SP, TOK_DEV).transpose(1, 0, 2), gate_in.astype(jnp.float32).reshape(N_SP, TOK_DEV, INNER), entry_states, mix_cot.reshape(N_SP, TOK_DEV, INNER))
    _, (mixed_all, grad_val, grad_key, grad_query, grad_dec, grad_gate_seg) = lax.scan(segment_step, jnp.zeros((HEADS, HEAD_DIM, NSTATE), jnp.float32), segment_inputs, reverse=True)
    mixer_out = mixed_all.reshape(TOKENS, INNER).astype(jnp.bfloat16)
    grad_out_weight = jnp.dot(grad_hidden.T, mixer_out, preferred_element_type=jnp.float32)
    grad_values = grad_val.reshape(TOKENS, INNER).astype(jnp.bfloat16)
    grad_key_side = grad_key.reshape(TOKENS, GROUPS * NSTATE).astype(jnp.bfloat16)
    grad_query_side = grad_query.reshape(TOKENS, GROUPS * NSTATE).astype(jnp.bfloat16)
    grad_decay = grad_dec.transpose(1, 0, 2).reshape(HEADS, TOKENS)
    grad_gate_in = grad_gate_seg.reshape(TOKENS, INNER).astype(jnp.bfloat16)
    return (grad_hidden, grad_gate_weight, grad_up_weight, grad_down_weight, grad_out_weight, grad_values, grad_key_side, grad_query_side, grad_decay, grad_gate_in)
```

```python
import jax
import jax.numpy as jnp
from jax import lax
from jax.sharding import PartitionSpec as P

HEADS = 16
HEAD_DIM = 64
GROUPS = 4

precise = lax.Precision.HIGHEST
f32 = jnp.float32
bf16 = jnp.bfloat16


def mm(spec, a, b):
    return jnp.einsum(spec, a, b, preferred_element_type=f32)


def swap_tp(x):
    n = lax.axis_size("tp")
    return lax.ppermute(x, "tp", [(i, (i + 1) % n) for i in range(n)])


def route_slots(routes_dev, expert_count):
    flat_routes = routes_dev.reshape(-1)
    onehot = (flat_routes[:, None] == jnp.arange(expert_count, dtype=jnp.int32)[None, :]).astype(
        jnp.int32
    )
    earlier = jnp.cumsum(onehot, axis=0) - onehot
    return jnp.sum(earlier * onehot, axis=1)


def halving(part, order):
    devices = part.shape[0]
    bits = devices.bit_length() - 1
    me = lax.axis_index("sp")
    left = list(range(bits - 1, -1, -1))
    part = part.reshape((2,) * bits + part.shape[1:])
    for bit in order:
        axis = left.index(bit)
        mine = (me >> bit) & 1
        keep = lax.dynamic_index_in_dim(part, mine, axis, keepdims=False)
        send = lax.dynamic_index_in_dim(part, 1 - mine, axis, keepdims=False).astype(bf16)
        got = lax.ppermute(send, "sp", [(i, i ^ (1 << bit)) for i in range(devices)])
        part = keep + got.astype(f32)
        left.pop(axis)
    return part


def per_device(
    out_grad,
    routes,
    route_weights,
    routed_rows,
    gate_weight,
    up_weight,
    down_weight,
    values,
    key_side,
    query_side,
    decay_log,
    gate_in,
    entry_states,
    out_weight,
):
    devices = lax.axis_size("sp")
    tp = lax.axis_index("tp")
    length, width = out_grad.shape
    half = width // lax.axis_size("tp")
    capacity = routed_rows.shape[2]
    cap = (capacity + 7) // 8 * 8
    rows = devices * cap
    gate_weight, up_weight, down_weight = gate_weight[0], up_weight[0], down_weight[0]
    hidden = gate_weight.shape[1]

    def own(x, axis):
        return lax.dynamic_slice_in_dim(x, tp * half, half, axis)

    def other(x, axis):
        return lax.dynamic_slice_in_dim(x, (1 - tp) * half, half, axis)

    target = routes * cap + route_slots(routes, devices).reshape(routes.shape)
    row_ids = jnp.arange(rows, dtype=jnp.int32)
    match = row_ids[:, None, None] == target.T[None]
    select = jnp.any(match, axis=1).astype(bf16)
    row_weight = jnp.sum(jnp.where(match, route_weights.T[None], 0.0), axis=(1, 2))
    out_half = own(out_grad, 1)
    outgoing = (mm("rt,td->rd", select, out_half) * row_weight[:, None]).astype(bf16)
    arrived = lax.all_to_all(outgoing, "sp", split_axis=0, concat_axis=0, tiled=True)

    saved = jnp.pad(routed_rows[0], ((0, 0), (0, cap - capacity), (0, 0))).reshape(rows, width)
    gate_pre = mm("rd,df->rf", saved, gate_weight)
    up_pre = mm("rd,df->rf", saved, up_weight)
    joined = jnp.concatenate([gate_weight, up_weight], axis=1)
    joined_own, joined_other = own(joined, 0), other(joined, 0)
    down_own, down_other = own(down_weight, 1), other(down_weight, 1)
    act = (jax.nn.silu(gate_pre) * up_pre).astype(bf16)

    heads = decay_log.shape[0]
    per_group = HEADS // GROUPS
    groups = heads // per_group

    def by_head(x):
        return x.reshape(length, groups, per_group, HEAD_DIM).transpose(1, 2, 0, 3)

    def by_token(x):
        return x.transpose(2, 0, 1, 3).reshape(length, heads * HEAD_DIM)

    key = key_side.reshape(length, groups, -1).transpose(1, 0, 2)
    query = query_side.reshape(length, groups, -1).transpose(1, 0, 2)
    nstate = key.shape[2]
    value = by_head(values)
    entry = entry_states[0].reshape(groups, per_group, HEAD_DIM, nstate)
    entry_b = entry.astype(bf16)
    steps = jnp.arange(length)
    causal = steps[:, None] >= steps[None, :]
    tri = causal.astype(f32)
    cum = jnp.einsum("hu,tu->ht", decay_log, tri, precision=precise)
    total = cum[:, -1]
    spread = cum[:, :, None] - cum[:, None, :]
    weights = jnp.where(causal, jnp.exp(jnp.where(causal, spread, 0.0)), 0.0)
    weights = weights.reshape(groups, per_group, length, length)
    cum4 = cum.reshape(groups, per_group, length, 1)
    growth = jnp.exp(cum4)
    tail = jnp.exp(total.reshape(groups, per_group, 1, 1) - cum4)
    scores = mm("gtn,gsn->gts", query, key)
    mix = (scores[:, None] * weights).astype(bf16)
    within = mm("grts,grsp->grtp", mix, value)
    carried = growth * mm("gtn,grpn->grtp", query, entry_b)
    gate = by_head(gate_in).astype(f32)
    sig = jax.nn.sigmoid(gate)
    silu_gate = gate * sig
    core = within + carried
    core_slope = core * (sig * (1.0 + gate * (1.0 - sig)))
    mixer_out = by_token((core * silu_gate).astype(bf16))

    arrived, gate_pre, up_pre, act, saved, mix, weights, within, carried, core_slope, mixer_out, \
        silu_gate, joined_own, joined_other, down_own, down_other, value = \
        lax.optimization_barrier((
            arrived, gate_pre, up_pre, act, saved, mix, weights, within, carried, core_slope,
            mixer_out, silu_gate, joined_own, joined_other, down_own, down_other, value))

    arrived_other = swap_tp(arrived)
    act_grad = mm("rd,fd->rf", arrived, down_own)
    act_grad = act_grad + mm("rd,fd->rf", arrived_other, down_other)
    gate_sigmoid = jax.nn.sigmoid(gate_pre)
    gate_grad = (act_grad * up_pre * gate_sigmoid * (1.0 + gate_pre * (1.0 - gate_sigmoid))).astype(bf16)
    up_grad = (act_grad * (gate_pre * gate_sigmoid)).astype(bf16)
    both = jnp.concatenate([gate_grad, up_grad], axis=1)
    give = mm("rf,df->rd", both, joined_other).astype(bf16)
    got = swap_tp(give)
    keep = mm("rf,df->rd", both, joined_own).astype(bf16)
    half_back = (keep.astype(f32) + got.astype(f32)).astype(bf16)
    returned = lax.all_to_all(half_back, "sp", split_axis=0, concat_axis=0, tiled=True)

    cot_rows = jnp.where(
        tp == 0,
        jnp.concatenate([arrived, arrived_other], axis=1),
        jnp.concatenate([arrived_other, arrived], axis=1),
    )
    grad_down = mm("rf,rd->fd", act, cot_rows).astype(bf16)
    grad_gate = mm("rd,rf->df", saved, gate_grad).astype(bf16)
    grad_up = mm("rd,rf->df", saved, up_grad).astype(bf16)
    returned, grad_down, grad_gate, grad_up = lax.optimization_barrier(
        (returned, grad_down, grad_gate, grad_up)
    )

    picked = mm("rt,rd->td", select, returned)
    hidden_half = (out_half.astype(f32) + picked).astype(bf16)
    grad_hidden = lax.all_gather(hidden_half, "tp", axis=1, tiled=True)

    mix_cot = by_head(mm("td,di->ti", grad_hidden, out_weight))
    cot = mix_cot * silu_gate
    cot_b = cot.astype(bf16)
    cot_r = cot_b.astype(f32)
    grown = (growth * cot_r).astype(bf16)
    entry_grad = mm("grtp,gtn->grpn", grown, query)

    piece = entry_grad.reshape(heads, devices, HEAD_DIM // devices * nstate).transpose(1, 0, 2)
    totals = jnp.broadcast_to(total[None, :, None], (devices, heads, 1))
    piece = jnp.concatenate([piece, totals], axis=2)
    piece = lax.all_to_all(piece, "sp", split_axis=0, concat_axis=0, tiled=True)

    share = mm("td,ti->di", grad_hidden, mixer_out)
    share, cot_b = lax.optimization_barrier((share, cot_b))
    split = share.shape[1] // 2
    blocks = share.reshape(devices, width // devices, share.shape[1])
    bits = devices.bit_length() - 1
    orders = list(range(bits)), list(range(bits))
    mid = bits // 2 - 1
    orders[1][0], orders[1][mid] = orders[1][mid], orders[1][0]
    grad_out = jnp.concatenate(
        [halving(blocks[:, :, :split], orders[0]), halving(blocks[:, :, split:], orders[1])], axis=1
    )

    piece, all_total = piece[:, :, :-1], piece[:, :, -1]
    seg = jnp.arange(devices)
    between = (seg[None, None, :] > seg[:, None, None]) & (seg[None, None, :] < seg[None, :, None])
    chain = jnp.einsum("jik,kh->hji", between.astype(f32), all_total, precision=precise)
    chain = jnp.where((seg[None, :] > seg[:, None])[None], jnp.exp(chain), 0.0)
    chained = jnp.einsum("hji,ihx->jhx", chain, piece, precision=precise)
    chained = lax.all_to_all(chained, "sp", split_axis=0, concat_axis=0, tiled=True)
    state = chained.transpose(1, 0, 2).reshape(groups, per_group, HEAD_DIM, nstate)
    state_b = state.astype(bf16)

    grad_gate_in = by_token((mix_cot * core_slope).astype(bf16))
    mix_grad = mm("grtp,grsp->grts", cot_b, value)
    score_grad = jnp.sum(mix_grad * weights, axis=1).astype(bf16)
    query_grad = mm("gts,gsn->gtn", score_grad, key) + mm("grtp,grpn->gtn", grown, entry_b)
    key_grad = mm("gts,gtn->gsn", score_grad, query)
    value_f = value.astype(f32)
    value_grad = mm("grts,grtp->grsp", mix, cot_b)
    decay_rows = jnp.sum(cot_r * within + cot * carried - value_f * value_grad, axis=3)

    value_tail = tail * mm("gsn,grpn->grsp", key, state_b)
    key_grad = key_grad + mm("grsp,grpn->gsn", (tail * value_f).astype(bf16), state_b)
    tail_rows = jnp.sum(value_f * value_tail, axis=3)
    last = jnp.exp(total) * jnp.sum(entry * state, axis=(2, 3)).reshape(heads)
    grad_decay = jnp.einsum(
        "ht,tu->hu", (decay_rows - tail_rows).reshape(heads, length), tri, precision=precise
    )
    grad_decay = grad_decay + (jnp.sum(tail_rows, axis=2).reshape(heads) + last)[:, None]
    flat = lambda x: x.transpose(1, 0, 2).reshape(length, groups * nstate).astype(bf16)
    return (
        grad_hidden,
        grad_gate[None],
        grad_up[None],
        grad_down[None],
        grad_out,
        by_token((value_grad + value_tail).astype(bf16)),
        flat(key_grad),
        flat(query_grad),
        grad_decay,
        grad_gate_in,
    )


def solution(mesh):
    in_specs = (
        P("sp", None),
        P("sp", None),
        P("sp", None),
        P("sp", None, None, None),
        P("sp", None, "tp"),
        P("sp", None, "tp"),
        P("sp", "tp", None),
        P("sp", "tp"),
        P("sp", "tp"),
        P("sp", "tp"),
        P("tp", "sp"),
        P("sp", "tp"),
        P("sp", "tp", None, None),
        P(None, "tp"),
    )
    out_specs = (
        P("sp", None),
        P("sp", None, "tp"),
        P("sp", None, "tp"),
        P("sp", "tp", None),
        P("sp", "tp"),
        P("sp", "tp"),
        P("sp", "tp"),
        P("sp", "tp"),
        P("tp", "sp"),
        P("sp", "tp"),
    )
    return jax.shard_map(
        per_device, mesh=mesh, in_specs=in_specs, out_specs=out_specs, check_vma=False
    )
```
